32 devices in a mesh: fs: 8 (over z, y), tp: 4 (over x, core).
Axes of the slice: x: 2, y: 2, z: 4, core: 2. Of those that a mesh axis runs over, the one named last changes fastest.
Arguments:
- layer_input: bfloat16 [6144, 2048], P('fs', 'tp'), may hold values from -6 to 6
- out_cotangent: bfloat16 [6144, 2048], P('fs', 'tp'), may hold values from -6 to 6
- gate_matrix: bfloat16 [2048, 6144], P('fs', 'tp'), may hold values from -0.125 to 0.125
- up_matrix: bfloat16 [2048, 6144], P('fs', 'tp'), may hold values from -0.125 to 0.125
- down_matrix: bfloat16 [6144, 2048], P('tp', 'fs'), may hold values from -0.078125 to 0.078125
Outputs:
- input_grad: bfloat16 [6144, 2048], P('fs', 'tp')
- gate_grad: float32 [2048, 6144], P('fs', 'tp')
- up_grad: float32 [2048, 6144], P('fs', 'tp')
- down_grad: float32 [6144, 2048], P('tp', 'fs')
The draws below stay inside these ranges and needn't reach their ends.
All inputs are finite; a program needn't handle non-finite values.
Results may differ from the reference program's by a relative error of at most 0.014.
Values may be sent and summed in bfloat16 or wider, within the bound.
A program may use at most 128 MiB of HBM per device.

```python
import jax
import jax.numpy as jnp

D = 2048
FF = 6144
TOKENS = 6144
N_TP = 4


def raised(array, key, source, target, parts, factor):
    def block_of(dim):
        return (jnp.arange(array.shape[dim]) // (array.shape[dim] // parts)).reshape((-1,) + (1,) * (array.ndim - 1 - dim))

    one_side = jax.random.permutation(key, parts)[block_of(target)]
    other_side = (block_of(target) + parts // 2) % parts
    return jnp.where((block_of(source) == one_side) | (block_of(source) == other_side), factor * array, array)


def levels(stream_key, shape, split, least, largest):
    factor_of = 1.0
    for dim, shards_of in split:
        heights = jax.random.uniform(jax.random.fold_in(jax.random.fold_in(stream_key, 6), dim), (shards_of,), jnp.float32, least / len(split), largest / len(split))
        factor_of = factor_of * jnp.repeat(jnp.exp(heights), shape[dim] // shards_of).reshape((-1,) + (1,) * (len(shape) - 1 - dim))
    return factor_of


def gaussian(own_key, shape, scale, limit, split=(), kind=jnp.bfloat16):
    result = scale * jax.random.normal(own_key, shape, jnp.float32)
    if split:
        result = result * levels(own_key, shape, split, -0.22, 0.18)
    return jnp.clip(result, -limit, limit).astype(kind)


def noise_with(key, extent, spread, most, pieces, heavy, held_as=jnp.bfloat16):
    values = spread * jax.random.normal(key, extent, jnp.float32)
    if pieces:
        values = values * levels(key, extent, pieces, -0.22, 0.18)
    return jnp.clip(raised(values, jax.random.fold_in(key, 3), *heavy), -most, most).astype(held_as)


def setup_inputs(seed: int = 0) -> dict:
    key_of = jax.random.split(jax.random.key(seed), 6)
    layer_input = gaussian(key_of[0], (TOKENS, D), 1.0, 6.0, ((0, 8), (1, 4)))
    out_cotangent = noise_with(key_of[1], (TOKENS, D), 1.0, 6.0, ((0, 8), (1, 4)), (0, 1, 8, 2.0))
    gate_matrix = gaussian(key_of[2], (D, FF), D ** -0.5, 0.125, ((0, 8), (1, 4)))
    up_matrix = gaussian(key_of[3], (D, FF), D ** -0.5, 0.125, ((0, 8), (1, 4)))
    down_matrix = gaussian(key_of[4], (FF, D), FF ** -0.5, 0.078125, ((0, 4), (1, 8)))
    return dict(layer_input=layer_input, out_cotangent=out_cotangent, gate_matrix=gate_matrix, up_matrix=up_matrix, down_matrix=down_matrix)


def reference(layer_input, out_cotangent, gate_matrix, up_matrix, down_matrix):
    gate_pre = jnp.dot(layer_input, gate_matrix, preferred_element_type=jnp.float32)
    up_pre = jnp.dot(layer_input, up_matrix, preferred_element_type=jnp.float32)
    sigmoid_gate = jax.nn.sigmoid(gate_pre)
    activation = gate_pre * sigmoid_gate
    hidden = (activation * up_pre).astype(jnp.bfloat16)
    hidden_delta = jnp.dot(out_cotangent, down_matrix.T, preferred_element_type=jnp.float32)
    up_delta = (hidden_delta * activation).astype(jnp.bfloat16)
    gate_delta = (hidden_delta * up_pre * sigmoid_gate * (1.0 + gate_pre * (1.0 - sigmoid_gate))).astype(jnp.bfloat16)
    gate_grad = jnp.dot(layer_input.T, gate_delta, preferred_element_type=jnp.float32)
    up_grad = jnp.dot(layer_input.T, up_delta, preferred_element_type=jnp.float32)
    down_grad = jnp.dot(hidden.T, out_cotangent, preferred_element_type=jnp.float32)
    block_width = FF // N_TP
    summed = jnp.zeros(layer_input.shape, jnp.float32)
    for block_index in range(N_TP):
        first_col = block_index * block_width
        last_col = first_col + block_width
        partial_value = jnp.dot(gate_delta[:, first_col:last_col], gate_matrix[:, first_col:last_col].T, preferred_element_type=jnp.float32)
        partial_value = partial_value + jnp.dot(up_delta[:, first_col:last_col], up_matrix[:, first_col:last_col].T, preferred_element_type=jnp.float32)
        summed = summed + partial_value.astype(jnp.bfloat16).astype(jnp.float32)
    return summed.astype(jnp.bfloat16), gate_grad, up_grad, down_grad
```

```python
import jax
import jax.numpy as jnp
import numpy as np
from jax import lax
from jax.sharding import PartitionSpec as P


def ring_order(n):
    return list(range(0, n, 2)) + list(range(n - 1, 0, -2))


def dot(left, right, dims):
    return lax.dot_general(left, right, (dims, ((), ())), preferred_element_type=jnp.float32)


NN = ((1,), (0,))
TN = ((0,), (0,))
NT = ((1,), (1,))


def make(n):
    order = ring_order(n)
    half = n // 2
    right = [(order[i], order[(i + 1) % n]) for i in range(n)]
    left = [(order[(i + 1) % n], order[i]) for i in range(n)]
    position = np.zeros(n, np.int32)
    position[order] = np.arange(n)
    order = np.asarray(order, np.int32)

    def go_right(value):
        return lax.ppermute(value, "fs", right)

    def go_left(value):
        return lax.ppermute(value, "fs", left)

    def after(value, *earlier):
        return lax.optimization_barrier((value, *earlier))[0]

    def gather(block):
        rel = [None] * n
        rel[0] = block
        from_left = from_right = block
        cut = block.shape[0] // 2
        for step in range(1, half):
            from_left = go_right(from_left)
            from_right = go_left(from_right)
            rel[n - step], rel[step] = from_left, from_right
            if step <= 2:
                early = (from_left, from_right)
        rel[half] = jnp.concatenate((go_right(from_left[:cut]), go_left(from_right[cut:])), axis=0)
        return jnp.concatenate(rel, axis=0), early

    def on_device(layer_input, out_cotangent, gate_matrix, up_matrix, down_matrix):
        me = jnp.asarray(position)[lax.axis_index("fs")]
        table = jnp.asarray(order)
        depth = gate_matrix.shape[0]

        gate, gate_hop = gather(gate_matrix)
        up, up_hop = gather(after(up_matrix, *gate_hop))
        down, _ = gather(after(down_matrix.T, *up_hop))

        def reordered(local):
            whole = lax.all_gather(local, "tp", axis=1, tiled=True)
            return jnp.concatenate(
                [
                    lax.dynamic_slice_in_dim(whole, table[(me + s) % n] * depth, depth, axis=1)
                    for s in range(n)
                ],
                axis=1,
            )

        x = reordered(layer_input)
        g = reordered(out_cotangent)

        def scatter(rows, delta):
            def term(step):
                first = (step % n) * depth
                return dot(rows[:, first : first + depth], delta, TN)

            far = term(half).astype(jnp.bfloat16)
            cut = depth // 2
            from_left = go_right(far[:cut])
            from_right = go_left(far[cut:])
            first_hop = (from_left, from_right)
            zeros = jnp.zeros_like(far[:cut])
            from_left = jnp.concatenate((from_left, zeros), axis=0)
            from_right = jnp.concatenate((zeros, from_right), axis=0)
            for step in range(half - 1, 0, -1):
                to_right = (term(step) + from_left.astype(jnp.float32)).astype(jnp.bfloat16)
                to_left = (term(-step) + from_right.astype(jnp.float32)).astype(jnp.bfloat16)
                from_left, from_right = go_right(to_right), go_left(to_left)
            total = term(0) + from_left.astype(jnp.float32) + from_right.astype(jnp.float32)
            return total, first_hop

        gate_pre = dot(x, gate, NN)
        up_pre = dot(x, up, NN)
        sigmoid_gate = jax.nn.sigmoid(gate_pre)
        activation = gate_pre * sigmoid_gate
        hidden = (activation * up_pre).astype(jnp.bfloat16)
        down_grad, _ = scatter(g, hidden)
        down_grad = down_grad.T
        hidden_delta = dot(after(g, hidden), down, NN)
        up_delta = (hidden_delta * activation).astype(jnp.bfloat16)
        gate_delta = (
            hidden_delta * up_pre * sigmoid_gate * (1.0 + gate_pre * (1.0 - sigmoid_gate))
        ).astype(jnp.bfloat16)

        gate_grad, gate_back = scatter(x, gate_delta)
        up_grad, up_back = scatter(x, up_delta)

        late_gate = after(gate_delta, *gate_back)
        late_up = after(up_delta, *up_back)
        partial_value = (dot(late_gate, gate, NT) + dot(late_up, up, NT)).astype(jnp.bfloat16)
        places = jnp.asarray(position)
        partial_value = jnp.concatenate(
            [
                lax.dynamic_slice_in_dim(
                    partial_value, ((places[j] - me + n) % n) * depth, depth, axis=1
                )
                for j in range(n)
            ],
            axis=1,
        )
        input_grad = lax.psum_scatter(partial_value, "tp", scatter_dimension=1, tiled=True)
        return input_grad, gate_grad, up_grad, down_grad

    return on_device


def solution(mesh):
    return jax.shard_map(
        make(mesh.shape["fs"]),
        mesh=mesh,
        in_specs=(P("fs", "tp"), P("fs", "tp"), P("fs", "tp"), P("fs", "tp"), P("tp", "fs")),
        out_specs=(P("fs", "tp"), P("fs", "tp"), P("fs", "tp"), P("tp", "fs")),
        check_vma=False,
    )
```

```python
import jax
import jax.numpy as jnp
import numpy as np
from jax import lax
from jax.sharding import PartitionSpec as P


def ring_order(n):
    return list(range(0, n, 2)) + list(range(n - 1, 0, -2))


def dot(left, right, dims):
    return lax.dot_general(left, right, (dims, ((), ())), preferred_element_type=jnp.float32)


NN = ((1,), (0,))
TN = ((0,), (0,))
NT = ((1,), (1,))


def make(n):
    order = ring_order(n)
    half = n // 2
    right = [(order[i], order[(i + 1) % n]) for i in range(n)]
    left = [(order[(i + 1) % n], order[i]) for i in range(n)]
    position = np.zeros(n, np.int32)
    position[order] = np.arange(n)
    order = np.asarray(order, np.int32)

    def go_right(value):
        return lax.ppermute(value, "fs", right)

    def go_left(value):
        return lax.ppermute(value, "fs", left)

    def after(value, *earlier):
        return lax.optimization_barrier((value, *earlier))[0]

    def gather(block):
        rel = [None] * n
        rel[0] = block
        from_left = from_right = block
        cut = block.shape[0] // 2
        for step in range(1, half):
            from_left = go_right(from_left)
            from_right = go_left(from_right)
            rel[n - step], rel[step] = from_left, from_right
            if step <= 2:
                early = (from_left, from_right)
        rel[half] = jnp.concatenate((go_right(from_left[:cut]), go_left(from_right[cut:])), axis=0)
        return jnp.concatenate(rel, axis=0), early

    def on_device(layer_input, out_cotangent, gate_matrix, up_matrix, down_matrix):
        me = jnp.asarray(position)[lax.axis_index("fs")]
        table = jnp.asarray(order)
        depth = gate_matrix.shape[0]

        gate, gate_hop = gather(gate_matrix)
        up, up_hop = gather(after(up_matrix, *gate_hop))
        down, _ = gather(after(down_matrix.T, *up_hop))

        def reordered(local):
            whole = lax.all_gather(local, "tp", axis=1, tiled=True)
            return jnp.concatenate(
                [
                    lax.dynamic_slice_in_dim(whole, table[(me + s) % n] * depth, depth, axis=1)
                    for s in range(n)
                ],
                axis=1,
            )

        x = reordered(layer_input)
        g = reordered(out_cotangent)

        def scatter(rows, delta):
            def term(step, delta):
                first = (step % n) * depth
                return dot(rows[:, first : first + depth], delta, TN)

            far = term(half, delta).astype(jnp.bfloat16)
            cut = depth // 2
            from_left = go_right(far[:cut])
            from_right = go_left(far[cut:])
            first_hop = (from_left, from_right)
            ready = delta
            zeros = jnp.zeros_like(far[:cut])
            from_left = jnp.concatenate((from_left, zeros), axis=0)
            from_right = jnp.concatenate((zeros, from_right), axis=0)
            for step in range(half - 1, 0, -1):
                to_right = (term(step, ready) + from_left.astype(jnp.float32)).astype(jnp.bfloat16)
                to_left = (term(-step, ready) + from_right.astype(jnp.float32)).astype(jnp.bfloat16)
                ready = after(delta, from_left, from_right)
                from_left, from_right = go_right(to_right), go_left(to_left)
            total = term(0, ready) + from_left.astype(jnp.float32) + from_right.astype(jnp.float32)
            return total, first_hop

        gate_pre = dot(x, gate, NN)
        up_pre = dot(x, up, NN)
        sigmoid_gate = jax.nn.sigmoid(gate_pre)
        activation = gate_pre * sigmoid_gate
        hidden = (activation * up_pre).astype(jnp.bfloat16)
        down_grad, _ = scatter(g, hidden)
        down_grad = down_grad.T
        hidden_delta = dot(after(g, hidden), down, NN)
        up_delta = (hidden_delta * activation).astype(jnp.bfloat16)
        gate_delta = (
            hidden_delta * up_pre * sigmoid_gate * (1.0 + gate_pre * (1.0 - sigmoid_gate))
        ).astype(jnp.bfloat16)

        gate_grad, gate_back = scatter(x, gate_delta)
        up_grad, up_back = scatter(x, up_delta)

        late_gate = after(gate_delta, *gate_back)
        late_up = after(up_delta, *up_back)
        partial_value = (dot(late_gate, gate, NT) + dot(late_up, up, NT)).astype(jnp.bfloat16)
        places = jnp.asarray(position)
        partial_value = jnp.concatenate(
            [
                lax.dynamic_slice_in_dim(
                    partial_value, ((places[j] - me + n) % n) * depth, depth, axis=1
                )
                for j in range(n)
            ],
            axis=1,
        )
        input_grad = lax.psum_scatter(partial_value, "tp", scatter_dimension=1, tiled=True)
        return input_grad, gate_grad, up_grad, down_grad

    return on_device


def solution(mesh):
    return jax.shard_map(
        make(mesh.shape["fs"]),
        mesh=mesh,
        in_specs=(P("fs", "tp"), P("fs", "tp"), P("fs", "tp"), P("fs", "tp"), P("tp", "fs")),
        out_specs=(P("fs", "tp"), P("fs", "tp"), P("fs", "tp"), P("tp", "fs")),
        check_vma=False,
    )
```
